32 devices in a mesh: sp: 16 (over z, y, x), tp: 2 (over core).
Axes of the slice: x: 2, y: 2, z: 4, core: 2. Of those that a mesh axis runs over, the one named last changes fastest.
Arguments:
- prompt: bfloat16 [16, 1024, 2048], P('sp', None, 'tp'), may hold values from -6 to 6
- new_input: bfloat16 [16, 2048], P('sp', 'tp'), may hold values from -140 to 140
- w_query: bfloat16 [2048, 2048], P('sp', 'tp'), may hold values from -0.21875 to 0.21875
- w_key: bfloat16 [2048, 2048], P('sp', 'tp'), may hold values from -0.125 to 0.125
- w_value: bfloat16 [2048, 2048], P('sp', 'tp'), may hold values from -0.125 to 0.125
- lam: float32 [16], P('tp'), may hold values from 0.3 to 0.8
- out_gain: float32 [128], replicated, may hold values from 0.1 to 1.9
Outputs:
- key_cache: bfloat16 [16, 1024, 2048], P('sp', None, 'tp')
- value_cache: bfloat16 [16, 1024, 2048], P('sp', None, 'tp')
- first_read: bfloat16 [16, 16, 128], P('sp', 'tp')
The draws below stay inside these ranges and needn't reach their ends.
All inputs are finite; a program needn't handle non-finite values.
Results may differ from the reference program's by a relative error of at most 0.02.
The reference program's roundings to bfloat16 on the way (of `query`) count: a program that leaves them out, or rounds other values in their place, can miss the bound.
Values may be sent and summed in bfloat16 or wider, within the bound.
A program may use at most 64 MiB of HBM per device.

```python
import jax
import jax.numpy as jnp
from jax import lax

WIDTH = 2048
HEADS = 16
MAP_DIM = 64
VAL_DIM = 128
LEN = 1024
SEQS = 16


def draw_new_input(key, part):
    values = jax.random.normal(key, (SEQS, WIDTH), jnp.float32)
    values = jnp.clip(values, -6.0, 6.0)
    return values.astype(jnp.bfloat16)


def levels(own_key, dims, shards, low, largest):
    gain = 1.0
    for dim, blocks in shards:
        draws = jax.random.uniform(jax.random.fold_in(jax.random.fold_in(own_key, 6), dim), (blocks,), jnp.float32, low / len(shards), largest / len(shards))
        gain = gain * jnp.repeat(jnp.exp(draws), dims[dim] // blocks).reshape((-1,) + (1,) * (len(dims) - 1 - dim))
    return gain


def gaussian(own_key, shape, width, reach, split=(), kind=jnp.bfloat16):
    level = levels(own_key, shape, split, -0.22, 0.18) if split else 1.0
    drawn = jax.random.normal(own_key, shape, jnp.float32) * width * level
    return jnp.minimum(jnp.maximum(drawn, -reach), reach).astype(kind)


def setup_inputs(seed: int = 0) -> dict:
    streams_of = jax.random.split(jax.random.key(seed), 8)
    prompt = gaussian(streams_of[0], (SEQS, LEN, WIDTH), 1.0, 6.0, ((0, 16), (2, 2)))
    new_input = draw_new_input(jax.random.fold_in(streams_of[7], 71), 0)
    w_query = gaussian(streams_of[2], (WIDTH, HEADS * 2 * MAP_DIM), (WIDTH // 3) ** -0.5, 0.21875, ((0, 16), (1, 2)))
    w_key = gaussian(streams_of[3], (WIDTH, HEADS * 2 * MAP_DIM), WIDTH ** -0.5, 0.125, ((0, 16), (1, 2)))
    w_value = gaussian(streams_of[4], (WIDTH, HEADS * VAL_DIM), WIDTH ** -0.5, 0.125, ((0, 16), (1, 2)))
    lam = jnp.clip(0.3 + 0.5 * jax.random.uniform(streams_of[5], (HEADS,), jnp.float32) ** levels(streams_of[5], (HEADS,), ((0, 2),), -0.2, 0.2), 0.3, 0.8)
    out_gain = jnp.clip(1.0 + 0.18 * jax.random.normal(streams_of[6], (VAL_DIM,), jnp.float32), 0.1, 1.9)
    return {"prompt": prompt, "new_input": new_input, "w_query": w_query, "w_key": w_key, "w_value": w_value, "lam": lam, "out_gain": out_gain}


rope_base = 500000.0
norm_eps = 1e-05

def rotate(vectors, angle):
    half = vectors.shape[-1] // 2
    cosine_table = jnp.cos(angle)
    sine = jnp.sin(angle)
    first = vectors[..., :half]
    second = vectors[..., half:]
    return jnp.concatenate([first * cosine_table - second * sine, second * cosine_table + first * sine], axis=-1)

def inverse_freq():
    return rope_base ** (-(jnp.arange(MAP_DIM // 2, dtype=jnp.float32) * 2.0 / MAP_DIM))

def reference(prompt, new_input, w_query, w_key, w_value, lam, out_gain):
    rows = prompt.reshape(SEQS * LEN, WIDTH)
    inverse = inverse_freq()
    positions = jnp.arange(LEN, dtype=jnp.float32)
    keys = jnp.dot(rows, w_key, preferred_element_type=jnp.float32).reshape(SEQS, LEN, HEADS, 2, MAP_DIM)
    keys = rotate(keys, positions[:, None, None, None] * inverse).astype(jnp.bfloat16)
    values = jnp.dot(rows, w_value, preferred_element_type=jnp.float32).astype(jnp.bfloat16)
    values = values.reshape(SEQS, LEN, HEADS, VAL_DIM)
    query = jnp.dot(new_input, w_query, preferred_element_type=jnp.float32).reshape(SEQS, HEADS, 2, MAP_DIM)
    query = rotate(query, jnp.float32(LEN) * inverse).astype(jnp.bfloat16)

    def single_sequence(args):
        single_head_query, single_head_keys, single_head_values = args
        attention_scores = jnp.einsum('fke,afke->fka', single_head_query.astype(jnp.float32), single_head_keys.astype(jnp.float32))
        weights = jax.nn.softmax(attention_scores * MAP_DIM ** (-0.5), axis=-1)
        mixed = jnp.einsum('hml,lhe->hme', weights, single_head_values.astype(jnp.float32), precision=lax.Precision.HIGHEST)
        diff = mixed[:, 0] - lam[:, None] * mixed[:, 1]
        normed = diff * lax.rsqrt(lax.optimization_barrier(jnp.mean(diff * diff, axis=-1, keepdims=True)) + norm_eps)
        return (normed * out_gain).astype(jnp.bfloat16)
    first_read = lax.map(single_sequence, (query, keys, values))
    return (keys.reshape(SEQS, LEN, HEADS * 2 * MAP_DIM), values.reshape(SEQS, LEN, HEADS * VAL_DIM), first_read)
```

```python
import functools

import jax
import jax.numpy as jnp
from jax import lax
from jax.experimental import pallas as pl
from jax.experimental.pallas import tpu as pltpu
from jax.sharding import PartitionSpec as P

MAP_DIM = 64
VAL_DIM = 128
LANES = 128
rope_base = 500000.0
norm_eps = 1e-05

X, Y, UP, DOWN = 0, 1, 2, 3
F32, BF16 = jnp.float32, jnp.bfloat16


def inverse_freq():
    return rope_base ** (-(jnp.arange(MAP_DIM // 2, dtype=F32) * 2.0 / MAP_DIM))


def tables(positions):
    angle = positions[:, None] * inverse_freq()
    cosine, sine = jnp.cos(angle), jnp.sin(angle)
    reps = LANES // MAP_DIM
    return (
        jnp.concatenate([cosine, cosine] * reps, axis=-1),
        jnp.concatenate([-sine, sine] * reps, axis=-1),
    )


def rotated(tile, cosine, sine):
    half = MAP_DIM // 2
    lane = lax.broadcasted_iota(jnp.int32, tile.shape, 1) % MAP_DIM
    other = jnp.where(lane < half, pltpu.roll(tile, LANES - half, 1), pltpu.roll(tile, half, 1))
    return tile * cosine + other * sine


def kernel(
    n, tp, prompt, fresh, wq, wk, wv, cos_t, sin_t, qcos, qsin, lam, gain,
    k_out, v_out, read_out,
    W, PR, acc, ko, vo, XN, XM, wq_v, QS, QR, ct, st,
    w_recv, w_send, p_recv, p_send, x_recv, x_send, xt_recv, xt_send, q_recv, q_send, loc,
):
    _, rows, wl = prompt.shape
    depth, cols = wk.shape
    half = cols // 2
    heads = cols // VAL_DIM
    L = n // 4
    plane = 4 * depth
    me, mt = lax.axis_index("sp"), lax.axis_index("tp")
    z, y, x = me // 4, (me // 2) % 2, me % 2
    yf, xf = 1 - y, 1 - x

    def at(zo, yo, xo):
        return zo * 4 + yo * 2 + xo

    partner = {X: at(z, y, xf), Y: at(z, yf, x), UP: me + 4, DOWN: me - 4}

    def piece(c, o):
        return W.at[c, pl.ds(pl.multiple_of(o * depth, depth), depth), :]

    def copy(c, d, o):
        return pltpu.make_async_remote_copy(
            src_ref=piece(c, o), dst_ref=piece(c, o),
            send_sem=w_send.at[(c * 4 + d) * n + o], recv_sem=w_recv.at[c * n + o],
            device_id={"sp": partner[d]}, device_id_type=pl.DeviceIdType.MESH,
        )

    def send(c, d, o):
        copy(c, d, o).start()

    def got(c, o):
        copy(c, X, o).wait_recv()

    barrier = pltpu.get_barrier_semaphore()
    for d in range(1, tp):
        pl.semaphore_signal(
            barrier, inc=1, device_id={"tp": (mt + d) % tp}, device_id_type=pl.DeviceIdType.MESH)

    def greet(d, _):
        pl.semaphore_signal(
            barrier, inc=1, device_id={"sp": (me + d) % n}, device_id_type=pl.DeviceIdType.MESH)
        return _

    lax.fori_loop(1, n, greet, 0)

    def columns(t):
        return PR.at[:, pl.ds(pl.multiple_of(t * wl, wl), wl)]

    own = [
        pltpu.make_async_copy(w.at[:, pl.ds(h * half, half)], piece(2 * i + h, me), loc.at[2 * i + h])
        for i, w in enumerate((wk, wv)) for h in range(2)
    ]
    rest = [
        pltpu.make_async_copy(fresh, XN.at[mt, me], loc.at[4]),
        pltpu.make_async_copy(prompt.at[0], columns(mt), loc.at[5]),
        pltpu.make_async_copy(wq, wq_v, loc.at[6]),
        pltpu.make_async_copy(cos_t, ct, loc.at[7]),
        pltpu.make_async_copy(sin_t, st, loc.at[8]),
    ]
    rest[0].start()
    for c in own:
        c.start()
    for c in rest[1:]:
        c.start()
    rest[0].wait()
    for c in own:
        c.wait()
    pl.semaphore_wait(barrier, n - 1 + tp - 1)

    def x_copy(d):
        return pltpu.make_async_remote_copy(
            src_ref=XN.at[mt, me], dst_ref=XN.at[mt, me],
            send_sem=x_send.at[d], recv_sem=x_recv.at[me],
            device_id={"sp": (me + d) % n}, device_id_type=pl.DeviceIdType.MESH,
        )

    def x_wait(d):
        src = (me + d) % n
        return pltpu.make_async_remote_copy(
            src_ref=XN.at[mt, src], dst_ref=XN.at[mt, src],
            send_sem=x_send.at[d], recv_sem=x_recv.at[src],
            device_id={"sp": src}, device_id_type=pl.DeviceIdType.MESH,
        )

    def loop(lo, hi, f):
        lax.fori_loop(lo, hi, lambda i, _: (f(i), _)[1], 0)

    loop(1, n, lambda d: x_copy(d).start())

    up_ok, down_ok = z + 1 < L, z > 0

    def along_z(c, o):
        @pl.when(up_ok)
        def _():
            send(c, UP, o)

        @pl.when(down_ok)
        def _():
            send(c, DOWN, o)

    send(0, Y, me)
    send(1, X, me)
    for c in range(4):
        along_z(c, me)
    send(2, X, me)
    send(3, Y, me)
    send(0, X, me)
    send(1, Y, me)
    send(2, Y, me)
    send(3, X, me)

    def p_copy(d):
        return pltpu.make_async_remote_copy(
            src_ref=prompt.at[0], dst_ref=columns(mt),
            send_sem=p_send.at[d], recv_sem=p_recv.at[mt],
            device_id={"tp": (mt + d) % tp}, device_id_type=pl.DeviceIdType.MESH,
        )

    def p_wait(d):
        src = (mt + d) % tp
        return pltpu.make_async_remote_copy(
            src_ref=columns(src), dst_ref=columns(src),
            send_sem=p_send.at[d], recv_sem=p_recv.at[src],
            device_id={"tp": src}, device_id_type=pl.DeviceIdType.MESH,
        )

    for d in range(1, tp):
        p_copy(d).start()

    o_y, o_x = at(z, yf, x), at(z, y, xf)
    got(0, o_y)
    along_z(0, o_y)
    send(0, X, o_y)
    got(1, o_x)
    along_z(1, o_x)
    send(1, Y, o_x)

    loop(1, n, lambda d: x_wait(d).wait_recv())

    def xt_copy(d, t):
        return pltpu.make_async_remote_copy(
            src_ref=XN.at[t], dst_ref=XN.at[t],
            send_sem=xt_send.at[d], recv_sem=xt_recv.at[t],
            device_id={"tp": (mt + d) % tp}, device_id_type=pl.DeviceIdType.MESH,
        )

    for d in range(1, tp):
        xt_copy(d, mt).start()
    for d in range(1, tp):
        xt_copy(d, (mt + d) % tp).wait_recv()
    first = me * depth
    holder, offset = first // wl, first % wl
    for j in range(n):
        XM[pl.ds(j, 1), :] = XN[holder, j]
    pick = (
        lax.broadcasted_iota(jnp.int32, (wl, depth), 0)
        == offset + lax.broadcasted_iota(jnp.int32, (wl, depth), 1)
    )
    chosen = jnp.dot(
        XM[...].astype(BF16), jnp.where(pick, 1.0, 0.0).astype(BF16), preferred_element_type=F32
    ).astype(BF16)
    rest[2].wait()
    partial = jnp.dot(chosen, wq_v[...], preferred_element_type=F32)
    for j in range(n):
        QS[j] = partial[j:j + 1, :]
    QR[me] = QS[me]

    def zero(i):
        acc[i // (rows // 128), pl.ds(pl.multiple_of((i % (rows // 128)) * 128, 128), 128), :] = (
            jnp.zeros((128, half), F32))

    loop(0, 4 * (rows // 128), zero)

    got(2, o_x)
    send(2, Y, o_x)
    got(3, o_y)
    send(3, X, o_y)

    def q_copy(d):
        dst = (me + d) % n
        return pltpu.make_async_remote_copy(
            src_ref=QS.at[dst], dst_ref=QR.at[me],
            send_sem=q_send.at[d], recv_sem=q_recv.at[me],
            device_id={"sp": dst}, device_id_type=pl.DeviceIdType.MESH,
        )

    def q_wait(d):
        src = (me + d) % n
        return pltpu.make_async_remote_copy(
            src_ref=QS.at[src], dst_ref=QR.at[src],
            send_sem=q_send.at[d], recv_sem=q_recv.at[src],
            device_id={"sp": src}, device_id_type=pl.DeviceIdType.MESH,
        )

    loop(1, n, lambda d: q_copy(d).start())

    rest[1].wait()
    for d in range(1, tp):
        p_wait(d).wait_recv()

    zlist = ((0, 0, 0, X), (1, 0, 0, Y), (2, 0, 0, X), (3, 0, 0, Y), (0, 1, 0, X), (1, 0, 1, Y))

    def relay(s):
        for c, fy, fx, across in zlist:
            yo = yf if fy else y
            xo = xf if fx else x
            for zo, valid, more, d in ((z - s, z - s >= 0, up_ok, UP), (z + s, z + s < L, down_ok, DOWN)):
                @pl.when(valid)
                def _(c=c, zo=zo, more=more, d=d, yo=yo, xo=xo, across=across):
                    o = at(zo, yo, xo)
                    got(c, o)

                    @pl.when(more)
                    def _():
                        send(c, d, o)

                    send(c, across, o)
        for zo, valid in ((z - s, z - s >= 0), (z + s, z + s < L)):
            @pl.when(valid)
            def _(zo=zo):
                send(2, Y, at(zo, y, x))
                send(3, X, at(zo, y, x))
                got(2, at(zo, y, xf))
                send(2, Y, at(zo, y, xf))
                got(3, at(zo, yf, x))
                send(3, X, at(zo, yf, x))

    R = min(rows, 256)

    def dots(zo):
        for c, order in ((0, ((y, xf), (yf, xf))), (1, ((yf, x), (yf, xf))),
                         (2, ((yf, x), (yf, xf))), (3, ((y, xf), (yf, xf)))):
            for yo, xo in order:
                got(c, at(zo, yo, xo))

        def tile(i):
            c, r = i // (rows // R), pl.ds(pl.multiple_of((i % (rows // R)) * R, R), R)
            p = pl.ds(pl.multiple_of(zo * plane, plane), plane)
            acc[c, r, :] += jnp.dot(PR[r, p], W[c, p, :], preferred_element_type=F32)

        loop(0, 4 * (rows // R), tile)

    def finish(s):
        @pl.when(z - s >= 0)
        def _():
            dots(z - s)

        @pl.when((z + s < L) & (s > 0))
        def _():
            dots(z + s)

    def step(s):
        relay(s)
        finish(s - 1)

    loop(1, L, step)

    loop(1, n, lambda d: q_wait(d).wait_recv())
    total = QR[0]
    for j in range(1, n):
        total = total + QR[j]
    total = jnp.broadcast_to(total, (8, cols))
    query = jnp.concatenate(
        [rotated(total[:, i:i + LANES], qcos[...], qsin[...]) for i in range(0, cols, LANES)], axis=1)
    maps = 2 * heads
    pad = max(maps, 16)
    query = jnp.broadcast_to(query[:1], (pad, cols))
    keep = (
        lax.broadcasted_iota(jnp.int32, (pad, cols), 0)
        == lax.broadcasted_iota(jnp.int32, (pad, cols), 1) // MAP_DIM
    )
    query = jnp.where(keep, query, 0.0).astype(BF16)
    rest[3].wait()
    rest[4].wait()

    finish(L - 1)

    def rotate_rows(i):
        r = pl.ds(pl.multiple_of(i * R, R), R)
        cosine, sine = ct[r, :], st[r, :]
        for j in range(0, cols, LANES):
            tile = acc[j // half, r, pl.ds(j % half, LANES)]
            ko[r, pl.ds(j, LANES)] = rotated(tile, cosine, sine).astype(BF16)

    loop(0, rows // R, rotate_rows)

    def value_rows(i):
        r = pl.ds(pl.multiple_of(i * R, R), R)
        for h in range(2):
            vo[r, pl.ds(h * half, half)] = acc[2 + h, r, :].astype(BF16)

    loop(0, rows // R, value_rows)
    k_copy = pltpu.make_async_copy(ko, k_out.at[0], loc.at[0])
    v_copy = pltpu.make_async_copy(vo, v_out.at[0], loc.at[1])
    k_copy.start()
    v_copy.start()
    scores = lax.dot_general(
        query, ko[...], (((1,), (1,)), ((), ())), preferred_element_type=F32) * MAP_DIM ** -0.5
    weights = jnp.exp(scores - jnp.max(scores, axis=-1, keepdims=True))
    weights = weights / jnp.sum(weights, axis=-1, keepdims=True)
    high = weights.astype(BF16)
    left = weights - high.astype(F32)
    mid = left.astype(BF16)
    low = (left - mid.astype(F32)).astype(BF16)
    mixed = jnp.dot(jnp.concatenate([high, mid, low], axis=0), vo[...], preferred_element_type=F32)
    mixed = mixed[:pad] + mixed[pad:2 * pad] + mixed[2 * pad:]
    for h in range(heads):
        c = slice(h * VAL_DIM, (h + 1) * VAL_DIM)
        diff = mixed[2 * h:2 * h + 1, c] - lam[h] * mixed[2 * h + 1:2 * h + 2, c]
        normed = diff * lax.rsqrt(jnp.mean(diff * diff, axis=-1, keepdims=True) + norm_eps)
        read_out[0, pl.ds(h, 1), :] = normed * gain[...]
    k_copy.wait()
    v_copy.wait()

    loop(1, n, lambda d: x_copy(d).wait_send())
    loop(1, n, lambda d: q_copy(d).wait_send())
    for d in range(1, tp):
        p_copy(d).wait_send()
        xt_copy(d, mt).wait_send()
    copy(0, Y, me).wait_send()
    copy(1, X, me).wait_send()

    def sent(zo):
        a, ay, ax = at(zo, y, x), at(zo, yf, x), at(zo, y, xf)
        for c, o in ((0, a), (0, ay), (2, a), (3, a), (3, ay)):
            copy(c, X, o).wait_send()
        for c, o in ((1, a), (1, ax), (3, a), (2, a), (2, ax)):
            copy(c, Y, o).wait_send()
        for ok, d in ((up_ok & (zo <= z), UP), (down_ok & (zo >= z), DOWN)):
            @pl.when(ok)
            def _(d=d):
                for c, o in ((0, a), (0, ay), (1, a), (1, ax), (2, a), (3, a)):
                    copy(c, d, o).wait_send()

    loop(0, L, sent)


def body(n, tp, prompt, new_input, w_query, w_key, w_value, lam, out_gain):
    seqs, rows, wl = prompt.shape
    depth, cols = w_key.shape
    heads = lam.shape[0]
    half = cols // 2
    cos_t, sin_t = tables(jnp.arange(rows, dtype=F32))
    qcos, qsin = tables(jnp.full((1,), rows, F32))
    any_ = pl.BlockSpec(memory_space=pl.ANY)
    vmem = pl.BlockSpec(memory_space=pltpu.VMEM)
    smem = pl.BlockSpec(memory_space=pltpu.SMEM)
    dma = pltpu.SemaphoreType.DMA
    keys, values, read = pl.pallas_call(
        functools.partial(kernel, n, tp),
        out_shape=(
            jax.ShapeDtypeStruct((seqs, rows, cols), BF16),
            jax.ShapeDtypeStruct((seqs, rows, cols), BF16),
            jax.ShapeDtypeStruct((seqs, heads, VAL_DIM), F32),
        ),
        in_specs=[any_] * 7 + [vmem, vmem, smem, vmem],
        out_specs=(any_, any_, vmem),
        scratch_shapes=[
            pltpu.VMEM((4, n * depth, half), BF16),
            pltpu.VMEM((rows, tp * wl), BF16),
            pltpu.VMEM((4, rows, half), F32),
            pltpu.VMEM((rows, cols), BF16),
            pltpu.VMEM((rows, cols), BF16),
            pltpu.VMEM((tp, n, 1, wl), F32),
            pltpu.VMEM((n, wl), F32),
            pltpu.VMEM((depth, cols), BF16),
            pltpu.VMEM((n, 1, cols), F32),
            pltpu.VMEM((n, 1, cols), F32),
            pltpu.VMEM((rows, LANES), F32),
            pltpu.VMEM((rows, LANES), F32),
            dma((4 * n,)), dma((16 * n,)), dma((tp,)), dma((tp,)), dma((n,)), dma((n,)),
            dma((tp,)), dma((tp,)), dma((n,)), dma((n,)), dma((9,)),
        ],
        compiler_params=pltpu.CompilerParams(
            collective_id=0, has_side_effects=True, vmem_limit_bytes=56 * 1024 * 1024),
        name="prefill",
    )(
        prompt, new_input.astype(F32), w_query, w_key, w_value, cos_t, sin_t,
        jnp.broadcast_to(qcos, (8, LANES)), jnp.broadcast_to(qsin, (8, LANES)), lam, out_gain[None, :],
    )
    return keys, values, read.astype(BF16)


def solution(mesh):
    in_specs = (
        P("sp", None, "tp"), P("sp", "tp"), P("sp", "tp"), P("sp", "tp"), P("sp", "tp"), P("tp"), P(),
    )
    out_specs = (P("sp", None, "tp"), P("sp", None, "tp"), P("sp", "tp", None))
    return jax.shard_map(
        functools.partial(body, mesh.shape["sp"], mesh.shape["tp"]),
        mesh=mesh, in_specs=in_specs, out_specs=out_specs, check_vma=False)
```

```python
import functools

import jax
import jax.numpy as jnp
from jax import lax
from jax.experimental import pallas as pl
from jax.experimental.pallas import tpu as pltpu
from jax.sharding import PartitionSpec as P

MAP_DIM = 64
VAL_DIM = 128
LANES = 128
rope_base = 500000.0
norm_eps = 1e-05

X, Y, UP, DOWN = 0, 1, 2, 3
F32, BF16 = jnp.float32, jnp.bfloat16


def inverse_freq():
    return rope_base ** (-(jnp.arange(MAP_DIM // 2, dtype=F32) * 2.0 / MAP_DIM))


def table(position, inverse):
    angle = position * inverse
    lane = lax.broadcasted_iota(jnp.int32, angle.shape, 1) % MAP_DIM
    sine = jnp.sin(angle)
    return jnp.cos(angle), jnp.where(lane < MAP_DIM // 2, -sine, sine)


def rotated(tile, cosine, sine):
    half = MAP_DIM // 2
    lane = lax.broadcasted_iota(jnp.int32, tile.shape, 1) % MAP_DIM
    other = jnp.where(lane < half, pltpu.roll(tile, LANES - half, 1), pltpu.roll(tile, half, 1))
    return tile * cosine + other * sine


def kernel(
    n, tp, prompt, fresh, wq, wk, wv, inverse,
    k_out, v_out, q_out,
    W, PR, acc, ko, vo, fr, XN, XM, wq_v, QS, QR, ct, st,
    w_recv, w_send, p_recv, p_send, x_recv, x_send, xt_recv, xt_send, q_recv, q_send, loc, token,
):
    _, rows, wl = prompt.shape
    depth, cols = wk.shape
    half = cols // 2
    heads = cols // VAL_DIM
    L = n // 4
    plane = 4 * depth
    me, mt = lax.axis_index("sp"), lax.axis_index("tp")
    z, y, x = me // 4, (me // 2) % 2, me % 2
    yf, xf = 1 - y, 1 - x

    def at(zo, yo, xo):
        return zo * 4 + yo * 2 + xo

    partner = {X: at(z, y, xf), Y: at(z, yf, x), UP: me + 4, DOWN: me - 4}

    def piece(c, o):
        return W.at[c, pl.ds(pl.multiple_of(o * depth, depth), depth), :]

    def copy(c, d, o):
        return pltpu.make_async_remote_copy(
            src_ref=piece(c, o), dst_ref=piece(c, o),
            send_sem=w_send.at[(c * 4 + d) * n + o], recv_sem=w_recv.at[c * n + o],
            device_id={"sp": partner[d]}, device_id_type=pl.DeviceIdType.MESH,
        )

    def send(c, d, o):
        copy(c, d, o).start()

    def got(c, o):
        copy(c, X, o).wait_recv()

    barrier = pltpu.get_barrier_semaphore()
    for d in range(1, tp):
        pl.semaphore_signal(
            barrier, inc=1, device_id={"tp": (mt + d) % tp}, device_id_type=pl.DeviceIdType.MESH)

    up_ok, down_ok = z + 1 < L, z > 0

    def signal(sem, d):
        pl.semaphore_signal(
            sem, inc=1, device_id={"sp": partner[d]}, device_id_type=pl.DeviceIdType.MESH)

    signal(barrier, X)
    signal(barrier, Y)
    pl.when(up_ok)(lambda: signal(barrier, UP))
    pl.when(down_ok)(lambda: signal(barrier, DOWN))

    def columns(t):
        return PR.at[:, pl.ds(pl.multiple_of(t * wl, wl), wl)]

    own = [
        pltpu.make_async_copy(w.at[:, pl.ds(h * half, half)], piece(2 * i + h, me), loc.at[2 * i + h])
        for i, w in enumerate((wk, wv)) for h in range(2)
    ]
    rest = [
        pltpu.make_async_copy(fresh, fr, loc.at[4]),
        pltpu.make_async_copy(prompt.at[0], columns(mt), loc.at[5]),
        pltpu.make_async_copy(wq, wq_v, loc.at[6]),
    ]
    rest[0].start()
    for c in own:
        c.start()
    for c in rest[1:]:
        c.start()
    rest[0].wait()
    XN[mt, me] = fr[...].astype(F32)
    for c in own:
        c.wait()

    @pl.when(up_ok & down_ok)
    def _():
        pl.semaphore_wait(barrier, 4 + tp - 1)

    @pl.when(jnp.logical_not(up_ok & down_ok))
    def _():
        pl.semaphore_wait(barrier, 3 + tp - 1)

    signal(token.at[Y], Y)

    def x_copy(d):
        return pltpu.make_async_remote_copy(
            src_ref=XN.at[mt, me], dst_ref=XN.at[mt, me],
            send_sem=x_send.at[d], recv_sem=x_recv.at[me],
            device_id={"sp": (me + d) % n}, device_id_type=pl.DeviceIdType.MESH,
        )

    def x_wait(d):
        src = (me + d) % n
        return pltpu.make_async_remote_copy(
            src_ref=XN.at[mt, src], dst_ref=XN.at[mt, src],
            send_sem=x_send.at[d], recv_sem=x_recv.at[src],
            device_id={"sp": src}, device_id_type=pl.DeviceIdType.MESH,
        )

    def loop(lo, hi, f):
        lax.fori_loop(lo, hi, lambda i, _: (f(i), _)[1], 0)

    def along_z(c, o):
        @pl.when(up_ok)
        def _():
            send(c, UP, o)

        @pl.when(down_ok)
        def _():
            send(c, DOWN, o)

    send(0, Y, me)
    send(1, X, me)
    for c in (2, 3, 0, 1):
        along_z(c, me)
    send(2, X, me)
    send(3, Y, me)
    send(0, X, me)
    send(1, Y, me)
    send(2, Y, me)
    send(3, X, me)

    def p_copy(d):
        return pltpu.make_async_remote_copy(
            src_ref=prompt.at[0], dst_ref=columns(mt),
            send_sem=p_send.at[d], recv_sem=p_recv.at[mt],
            device_id={"tp": (mt + d) % tp}, device_id_type=pl.DeviceIdType.MESH,
        )

    def p_wait(d):
        src = (mt + d) % tp
        return pltpu.make_async_remote_copy(
            src_ref=columns(src), dst_ref=columns(src),
            send_sem=p_send.at[d], recv_sem=p_recv.at[src],
            device_id={"tp": src}, device_id_type=pl.DeviceIdType.MESH,
        )

    for d in range(1, tp):
        p_copy(d).start()

    pl.semaphore_wait(token.at[Y], 1)
    signal(token.at[X], X)
    pl.semaphore_wait(token.at[X], 1)
    for ok, more, d in ((down_ok, up_ok, UP), (up_ok, down_ok, DOWN)):
        @pl.when(ok)
        def _(d=d):
            pl.semaphore_wait(token.at[d], 1)

        @pl.when(more)
        def _(d=d):
            signal(token.at[d], d)
    loop(1, n, lambda d: x_copy(d).start())

    o_y, o_x = at(z, yf, x), at(z, y, xf)
    got(0, o_y)
    along_z(0, o_y)
    send(0, X, o_y)
    got(1, o_x)
    along_z(1, o_x)
    send(1, Y, o_x)

    loop(1, n, lambda d: x_wait(d).wait_recv())

    def xt_copy(d, t):
        return pltpu.make_async_remote_copy(
            src_ref=XN.at[t], dst_ref=XN.at[t],
            send_sem=xt_send.at[d], recv_sem=xt_recv.at[t],
            device_id={"tp": (mt + d) % tp}, device_id_type=pl.DeviceIdType.MESH,
        )

    for d in range(1, tp):
        xt_copy(d, mt).start()
    for d in range(1, tp):
        xt_copy(d, (mt + d) % tp).wait_recv()
    first = me * depth
    holder, offset = first // wl, first % wl
    for j in range(n):
        XM[pl.ds(j, 1), :] = XN[holder, j]
    pick = (
        lax.broadcasted_iota(jnp.int32, (wl, depth), 0)
        == offset + lax.broadcasted_iota(jnp.int32, (wl, depth), 1)
    )
    chosen = jnp.dot(
        XM[...].astype(BF16), jnp.where(pick, 1.0, 0.0).astype(BF16), preferred_element_type=F32
    ).astype(BF16)
    rest[2].wait()
    partial = jnp.dot(chosen, wq_v[...], preferred_element_type=F32)
    for j in range(n):
        QS[j] = partial[j:j + 1, :]
    QR[me] = QS[me]

    def zero(i):
        acc[i // (rows // 128), pl.ds(pl.multiple_of((i % (rows // 128)) * 128, 128), 128), :] = (
            jnp.zeros((128, half), F32))

    loop(0, 4 * (rows // 128), zero)

    def angles(i):
        position = (i * 64 + lax.broadcasted_iota(jnp.int32, (64, LANES), 0)).astype(F32)
        r = pl.ds(pl.multiple_of(i * 64, 64), 64)
        ct[r, :], st[r, :] = table(position, inverse[...])

    loop(0, rows // 64, angles)
    qcos, qsin = table(jnp.full((8, LANES), rows, F32), inverse[...])

    got(2, o_x)
    send(2, Y, o_x)
    got(3, o_y)
    send(3, X, o_y)

    def q_copy(d):
        dst = (me + d) % n
        return pltpu.make_async_remote_copy(
            src_ref=QS.at[dst], dst_ref=QR.at[me],
            send_sem=q_send.at[d], recv_sem=q_recv.at[me],
            device_id={"sp": dst}, device_id_type=pl.DeviceIdType.MESH,
        )

    def q_wait(d):
        src = (me + d) % n
        return pltpu.make_async_remote_copy(
            src_ref=QS.at[src], dst_ref=QR.at[src],
            send_sem=q_send.at[d], recv_sem=q_recv.at[src],
            device_id={"sp": src}, device_id_type=pl.DeviceIdType.MESH,
        )

    loop(1, n, lambda d: q_copy(d).start())

    rest[1].wait()
    for d in range(1, tp):
        p_wait(d).wait_recv()

    def relay(s):
        sides = ((z - s, z - s >= 0, up_ok, UP), (z + s, z + s < L, down_ok, DOWN))

        def along(c, yo, xo, across):
            for zo, valid, more, d in sides:
                @pl.when(valid)
                def _(zo=zo, more=more, d=d):
                    o = at(zo, yo, xo)
                    got(c, o)

                    @pl.when(more)
                    def _():
                        send(c, d, o)

                    for a in across:
                        send(c, a, o)

        along(2, y, x, (X, Y))
        along(3, y, x, (Y, X))
        along(0, y, x, (X,))
        along(1, y, x, (Y,))
        for zo, valid, _, _ in sides:
            @pl.when(valid)
            def _(zo=zo):
                got(2, at(zo, y, xf))
                send(2, Y, at(zo, y, xf))
                got(3, at(zo, yf, x))
                send(3, X, at(zo, yf, x))
        along(0, yf, x, (X,))
        along(1, y, xf, (Y,))

    R = min(rows, 256)

    def dots(zo):
        for c, order in ((2, ((yf, x), (yf, xf))), (3, ((y, xf), (yf, xf))),
                         (0, ((y, xf), (yf, xf))), (1, ((yf, x), (yf, xf)))):
            for yo, xo in order:
                got(c, at(zo, yo, xo))

            def tile(i, c=c):
                r = pl.ds(pl.multiple_of(i * R, R), R)
                p = pl.ds(pl.multiple_of(zo * plane, plane), plane)
                acc[c, r, :] += jnp.dot(PR[r, p], W[c, p, :], preferred_element_type=F32)

            loop(0, rows // R, tile)

    def finish(s):
        @pl.when(z - s >= 0)
        def _():
            dots(z - s)

        @pl.when((z + s < L) & (s > 0))
        def _():
            dots(z + s)

    def step(s):
        relay(s)
        finish(s - 1)

    loop(1, L, step)

    loop(1, n, lambda d: q_wait(d).wait_recv())
    total = QR[0]
    for j in range(1, n):
        total = total + QR[j]
    total = jnp.broadcast_to(total, (8, cols))
    query = jnp.concatenate(
        [rotated(total[:, i:i + LANES], qcos, qsin) for i in range(0, cols, LANES)], axis=1)
    maps = 2 * heads
    pad = max(maps, 16)
    query = jnp.broadcast_to(query[:1], (pad, cols))
    keep = (
        lax.broadcasted_iota(jnp.int32, (pad, cols), 0)
        == lax.broadcasted_iota(jnp.int32, (pad, cols), 1) // MAP_DIM
    )
    q_out[...] = jnp.where(keep, query, 0.0).astype(BF16)

    finish(L - 1)

    def rotate_rows(i):
        r = pl.ds(pl.multiple_of(i * R, R), R)
        cosine, sine = ct[r, :], st[r, :]
        for j in range(0, cols, LANES):
            tile = acc[j // half, r, pl.ds(j % half, LANES)]
            ko[r, pl.ds(j, LANES)] = rotated(tile, cosine, sine).astype(BF16)

    def value_rows(i):
        r = pl.ds(pl.multiple_of(i * R, R), R)
        for h in range(2):
            vo[r, pl.ds(h * half, half)] = acc[2 + h, r, :].astype(BF16)

    v_copy = pltpu.make_async_copy(vo, v_out.at[0], loc.at[1])
    k_copy = pltpu.make_async_copy(ko, k_out.at[0], loc.at[0])
    loop(0, rows // R, value_rows)
    v_copy.start()
    loop(0, rows // R, rotate_rows)
    k_copy.start()

    loop(1, n, lambda d: x_copy(d).wait_send())
    loop(1, n, lambda d: q_copy(d).wait_send())
    for d in range(1, tp):
        p_copy(d).wait_send()
        xt_copy(d, mt).wait_send()
    copy(0, Y, me).wait_send()
    copy(1, X, me).wait_send()

    def sent(zo):
        a, ay, ax = at(zo, y, x), at(zo, yf, x), at(zo, y, xf)
        for c, o in ((0, a), (0, ay), (2, a), (3, a), (3, ay)):
            copy(c, X, o).wait_send()
        for c, o in ((1, a), (1, ax), (3, a), (2, a), (2, ax)):
            copy(c, Y, o).wait_send()
        for ok, d in ((up_ok & (zo <= z), UP), (down_ok & (zo >= z), DOWN)):
            @pl.when(ok)
            def _(d=d):
                for c, o in ((0, a), (0, ay), (1, a), (1, ax), (2, a), (3, a)):
                    copy(c, d, o).wait_send()

    loop(0, L, sent)
    v_copy.wait()
    k_copy.wait()


def read(keys, values, query, lam, gain, k_out, v_out, read_out, ko, vo, sem):
    heads, pad = lam.shape[0], query.shape[0]
    v_in = pltpu.make_async_copy(values.at[0], vo, sem.at[1])
    k_in = pltpu.make_async_copy(keys.at[0], ko, sem.at[0])
    k_copy = pltpu.make_async_copy(ko, k_out.at[0], sem.at[2])
    v_copy = pltpu.make_async_copy(vo, v_out.at[0], sem.at[3])
    k_in.start()
    v_in.start()
    k_in.wait()
    k_copy.start()
    scores = lax.dot_general(
        query[...], ko[...], (((1,), (1,)), ((), ())), preferred_element_type=F32) * MAP_DIM ** -0.5
    weights = jnp.exp(scores - jnp.max(scores, axis=-1, keepdims=True))
    weights = weights / jnp.sum(weights, axis=-1, keepdims=True)
    high = weights.astype(BF16)
    left = weights - high.astype(F32)
    mid = left.astype(BF16)
    low = (left - mid.astype(F32)).astype(BF16)
    v_in.wait()
    v_copy.start()
    mixed = jnp.dot(jnp.concatenate([high, mid, low], axis=0), vo[...], preferred_element_type=F32)
    mixed = mixed[:pad] + mixed[pad:2 * pad] + mixed[2 * pad:]
    reads = []
    for h in range(heads):
        c = slice(h * VAL_DIM, (h + 1) * VAL_DIM)
        diff = mixed[2 * h:2 * h + 1, c] - lam[h] * mixed[2 * h + 1:2 * h + 2, c]
        normed = diff * lax.rsqrt(jnp.mean(diff * diff, axis=-1, keepdims=True) + norm_eps)
        reads.append(normed * gain[...])
    read_out[0] = jnp.concatenate(reads, axis=0).astype(BF16)
    k_copy.wait()
    v_copy.wait()


def body(n, tp, prompt, new_input, w_query, w_key, w_value, lam, out_gain):
    seqs, rows, wl = prompt.shape
    depth, cols = w_key.shape
    heads = lam.shape[0]
    half = cols // 2
    pad = max(2 * heads, 16)
    inverse = jnp.tile(inverse_freq(), LANES * 2 // MAP_DIM)[None, :]
    any_ = pl.BlockSpec(memory_space=pl.ANY)
    hbm = pl.BlockSpec(memory_space=pltpu.HBM)
    vmem = pl.BlockSpec(memory_space=pltpu.VMEM)
    smem = pl.BlockSpec(memory_space=pltpu.SMEM)
    dma = pltpu.SemaphoreType.DMA
    keys, values, query = pl.pallas_call(
        functools.partial(kernel, n, tp),
        out_shape=(
            jax.ShapeDtypeStruct((seqs, rows, cols), BF16),
            jax.ShapeDtypeStruct((seqs, rows, cols), BF16),
            jax.ShapeDtypeStruct((pad, cols), BF16),
        ),
        in_specs=[hbm] * 5 + [vmem],
        out_specs=(any_, any_, vmem),
        scratch_shapes=[
            pltpu.VMEM((4, n * depth, half), BF16),
            pltpu.VMEM((rows, tp * wl), BF16),
            pltpu.VMEM((4, rows, half), F32),
            pltpu.VMEM((rows, cols), BF16),
            pltpu.VMEM((rows, cols), BF16),
            pltpu.VMEM((1, wl), BF16),
            pltpu.VMEM((tp, n, 1, wl), F32),
            pltpu.VMEM((n, wl), F32),
            pltpu.VMEM((depth, cols), BF16),
            pltpu.VMEM((n, 1, cols), F32),
            pltpu.VMEM((n, 1, cols), F32),
            pltpu.VMEM((rows, LANES), F32),
            pltpu.VMEM((rows, LANES), F32),
            dma((4 * n,)), dma((16 * n,)), dma((tp,)), dma((tp,)), dma((n,)), dma((n,)),
            dma((tp,)), dma((tp,)), dma((n,)), dma((n,)), dma((7,)), pltpu.SemaphoreType.REGULAR((4,)),
        ],
        compiler_params=pltpu.CompilerParams(
            collective_id=0, has_side_effects=True, vmem_limit_bytes=40 * 1024 * 1024),
        name="prefill",
    )(prompt, new_input, w_query, w_key, w_value, inverse)
    return pl.pallas_call(
        read,
        out_shape=(
            jax.ShapeDtypeStruct((seqs, rows, cols), BF16),
            jax.ShapeDtypeStruct((seqs, rows, cols), BF16),
            jax.ShapeDtypeStruct((seqs, heads, VAL_DIM), BF16),
        ),
        in_specs=[any_, any_, vmem, smem, vmem],
        out_specs=(any_, any_, vmem),
        scratch_shapes=[pltpu.VMEM((rows, cols), BF16), pltpu.VMEM((rows, cols), BF16), dma((4,))],
        compiler_params=pltpu.CompilerParams(vmem_limit_bytes=24 * 1024 * 1024),
        name="read",
    )(keys, values, query, lam, out_gain[None, :])


def solution(mesh):
    in_specs = (
        P("sp", None, "tp"), P("sp", "tp"), P("sp", "tp"), P("sp", "tp"), P("sp", "tp"), P("tp"), P(),
    )
    out_specs = (P("sp", None, "tp"), P("sp", None, "tp"), P("sp", "tp", None))
    return jax.shard_map(
        functools.partial(body, mesh.shape["sp"], mesh.shape["tp"]),
        mesh=mesh, in_specs=in_specs, out_specs=out_specs, check_vma=False)
```
